32 devices in a mesh: grp: 2 (over y), fs: 4 (over z), tp: 4 (over x, core).
Axes of the slice: x: 2, y: 2, z: 4, core: 2. Of those that a mesh axis runs over, the one named last changes fastest.
Arguments:
- tokens: bfloat16 [2048, 2048], P(('grp', 'fs'), 'tp'), parts along dimension 0, may hold values from -6 to 6
- route_experts: int32 [2048, 2], P(('grp', 'fs')), parts along dimension 0, may hold values from 0 to 15, as said below
- group_weight: float32 [2048], P(('grp', 'fs')), parts along dimension 0, may hold values from 0.2 to 1
- pair_logit: float32 [2048], P(('grp', 'fs')), parts along dimension 0, may hold values from -6 to 6
- norm_gain: float32 [2048], replicated, may hold values from 0.1 to 1.9
- gate_train: float32 [16, 2048, 2048], P(None, 'fs', 'tp'), may hold values from -0.125 to 0.125
- up_train: float32 [16, 2048, 2048], P(None, 'fs', 'tp'), may hold values from -0.125 to 0.125
- down_train: float32 [16, 2048, 2048], P(None, 'fs', 'tp'), may hold values from -0.125 to 0.125
Outputs:
- gate_serve: bfloat16 [32, 2048, 2048], P(('grp', 'fs'), None, 'tp'), parts along dimension 0
- up_serve: bfloat16 [32, 2048, 2048], P(('grp', 'fs'), None, 'tp'), parts along dimension 0
- down_serve: bfloat16 [32, 2048, 2048], P(('grp', 'fs'), None, 'tp'), parts along dimension 0
- moe_out: bfloat16 [2048, 2048], P(('grp', 'fs'), 'tp'), parts along dimension 0
The draws below stay inside these ranges and needn't reach their ends.
There are 2 independent parts, one for each index of `grp`. The reference program is written for one: setup_inputs(seed, part) draws one part's arguments, and reference() takes and returns one part's arrays. A program takes and returns all parts, laid end to end along the dimension named above; an argument that names none is the same for every part. Nothing has to cross between parts.
Inputs may be any that keep to these rules, and one draw needn't show every extreme that they name: `route_experts`: each row names two different experts of the same group of 4 consecutive expert numbers. Among the 256 aligned rows of one index of fs, no expert is named by more than 64 rows, and in every draw some expert is named by exactly 64 rows from every such block.
All inputs are finite; a program needn't handle non-finite values.
Results may differ from the reference program's by a relative error of at most 0.018.
Values may be sent and summed in bfloat16 or wider, within the bound.
A program may use at most 192 MiB of HBM per device.

```python
import math
import jax
import jax.numpy as jnp
from jax import lax

D = 2048
FF = 2048
GROUPS = 4
PER_GROUP = 4
TOK_DEV = 256
EXPERTS = 16
CAP = 64
TOKENS = 1024
N_FS = 4
N_TP = 4


def draw_route_experts(key, part):
    blocks = TOKENS // TOK_DEV
    busiest = jax.random.randint(jax.random.fold_in(key, 7), (), 0, GROUPS)
    block_keys = jax.random.split(jax.random.fold_in(key, 11), blocks)
    group_ids = jnp.arange(GROUPS, dtype=jnp.int32)

    def one_block(block_key):
        cut_key, relabel_key, shuffle_key = jax.random.split(block_key, 3)
        remainder = TOK_DEV - 2 * CAP
        cut_points = jnp.sort(jax.random.randint(cut_key, (2,), 0, remainder + 1))
        others = jnp.stack([cut_points[0], cut_points[1] - cut_points[0], remainder - cut_points[1]])
        other_slot = jnp.minimum((group_ids - busiest - 1) % GROUPS, 2)
        counts = jnp.where(group_ids == busiest, 2 * CAP, others[other_slot])
        group_ends = jnp.cumsum(counts)
        group_starts = group_ends - counts
        positions = jnp.arange(TOK_DEV, dtype=jnp.int32)
        member = jnp.sum((positions[:, None] >= group_ends[None, :]).astype(jnp.int32), axis=1)
        member = jnp.minimum(member, GROUPS - 1)
        within = positions - group_starts[member]
        first_rank = within % PER_GROUP
        second = (first_rank + 1 + within // PER_GROUP % (PER_GROUP - 1)) % PER_GROUP

        def relabel_group(group):
            return jax.random.permutation(jax.random.fold_in(relabel_key, group), PER_GROUP)
        relabel = jax.vmap(relabel_group)(group_ids)
        chosen_pair = jnp.stack([member * PER_GROUP + relabel[member, first_rank], member * PER_GROUP + relabel[member, second]], axis=1)
        shuffle = jax.random.permutation(shuffle_key, TOK_DEV)
        return chosen_pair[shuffle]
    return jax.vmap(one_block)(block_keys).reshape(TOKENS, 2).astype(jnp.int32)


def shard_levels(key, shape, pieces, smallest, high):
    loudness = 1.0
    for position, blocks in pieces:
        draws = jax.random.uniform(jax.random.fold_in(jax.random.fold_in(key, 6), position), (blocks,), jnp.float32, smallest / len(pieces), high / len(pieces))
        loudness = loudness * jnp.repeat(jnp.exp(draws), shape[position] // blocks).reshape((-1,) + (1,) * (len(shape) - 1 - position))
    return loudness


def normal_values(own_key, shape, width, most, shards=(), kind=jnp.bfloat16):
    values = width * jax.random.normal(own_key, shape, jnp.float32)
    if shards:
        values = values * shard_levels(own_key, shape, shards, -0.22, 0.18)
    return jnp.clip(values, -most, most).astype(kind)


def setup_inputs(seed: int = 0, part: int = 0) -> dict:
    streams_of = jax.random.split(jax.random.key(seed), 9)
    own_keys = jax.random.split(jax.random.fold_in(streams_of[8], part), 9)
    return {
        "tokens": normal_values(own_keys[0], (TOKENS, D), 1.0, 6.0, ((0, 4), (1, 4))),
        "route_experts": draw_route_experts(jax.random.fold_in(jax.random.fold_in(streams_of[8], part), 71), part),
        "group_weight": jnp.clip(jnp.exp(math.log(1.0) - 1.609438 * jax.random.uniform(own_keys[2], (TOKENS,), jnp.float32) ** shard_levels(own_keys[2], (TOKENS,), ((0, 4),), -0.2, 0.2)), 0.2, 1.0),
        "pair_logit": normal_values(own_keys[3], (TOKENS,), 1.5, 6.0, ((0, 4),), jnp.float32),
        "norm_gain": jnp.clip(1.0 + 0.18 * jax.random.normal(streams_of[4], (D,), jnp.float32), 0.1, 1.9),
        "gate_train": normal_values(streams_of[5], (EXPERTS, D, FF), D ** -0.5, 0.125, ((1, 4), (2, 4)), jnp.float32),
        "up_train": normal_values(streams_of[6], (EXPERTS, D, FF), D ** -0.5, 0.125, ((1, 4), (2, 4)), jnp.float32),
        "down_train": normal_values(streams_of[7], (EXPERTS, D, FF), FF ** -0.5, 0.125, ((1, 4), (2, 4)), jnp.float32),
    }


def reference(tokens, route_experts, group_weight, pair_logit, norm_gain, gate_train, up_train, down_train):
    gate_serve = (norm_gain[None, :, None] * gate_train).astype(jnp.bfloat16)
    up_serve = (norm_gain[None, :, None] * up_train).astype(jnp.bfloat16)
    down_serve = down_train.astype(jnp.bfloat16)
    as_float = tokens.astype(jnp.float32)
    row_scale = lax.rsqrt(lax.optimization_barrier(jnp.mean(as_float * as_float, axis=1)) + 1e-06)
    first_gate = group_weight * jax.nn.sigmoid(pair_logit)
    second_gate = group_weight * jax.nn.sigmoid(-pair_logit)
    most_rows = N_FS * CAP
    block_width = FF // N_TP

    def add_expert(expert, running):
        first_hit = route_experts[:, 0] == expert
        second_hit = route_experts[:, 1] == expert
        row_weight = jnp.where(first_hit, first_gate, 0.0) + jnp.where(second_hit, second_gate, 0.0)
        sort_key = jnp.where(first_hit | second_hit, 0, 1).astype(jnp.int32)
        row_order = jnp.argsort(sort_key, stable=True)[:most_rows].astype(jnp.int32)
        picked = tokens[row_order]
        picked_scale = row_scale[row_order][:, None]
        gate_pre = picked_scale * jnp.dot(picked, gate_serve[expert], preferred_element_type=jnp.float32)
        up_pre = picked_scale * jnp.dot(picked, up_serve[expert], preferred_element_type=jnp.float32)
        hidden = (jax.nn.silu(gate_pre) * up_pre).astype(jnp.bfloat16)
        down_expert = down_serve[expert]

        def add_block(block, partial_sum):
            column = (block * block_width).astype(jnp.int32)
            hidden_part = lax.dynamic_slice_in_dim(hidden, column, block_width, 1)
            down_part = lax.dynamic_slice_in_dim(down_expert, column, block_width, 1)
            partial_value = jnp.dot(hidden_part, down_part.T, preferred_element_type=jnp.float32).astype(jnp.bfloat16)
            partial_value = lax.optimization_barrier(partial_value)
            return partial_sum + partial_value.astype(jnp.float32)
        summed = lax.fori_loop(0, N_TP, add_block, jnp.zeros((most_rows, D), jnp.float32))
        routed = lax.optimization_barrier(summed.astype(jnp.bfloat16)).astype(jnp.float32)
        return running.at[row_order].add(row_weight[row_order][:, None] * routed)
    total = lax.fori_loop(0, EXPERTS, add_expert, jnp.zeros((TOKENS, D), jnp.float32))
    return (gate_serve, up_serve, down_serve, total.astype(jnp.bfloat16))
```

```python
import functools

import jax
import jax.numpy as jnp
from jax import lax
from jax.experimental import pallas as pl
from jax.experimental.pallas import tpu as pltpu
from jax.sharding import PartitionSpec as P


CAP = 64
GROUP = 4
MESH = pl.DeviceIdType.MESH


def ring(size, shift):
    return [(i, (i + shift) % size) for i in range(size)]


def cast_block(train, gain, expert, experts, row, rows):
    block = lax.dynamic_slice(train, (expert, row, 0), (experts, rows, train.shape[2]))
    if gain is not None:
        block = lax.dynamic_slice_in_dim(gain, row, rows)[None, :, None] * block
    return block.astype(jnp.bfloat16)


def move(block, axis, shift):
    return lax.ppermute(block, axis, ring(lax.axis_size(axis), shift))


def tail_kernel(dims, hidden, down, pick, out, weights, relay_out, relay_in, relay_sum,
                own_out, own_in, own_sum, cross_out, cross_in, back_out, back_in, *sems):
    owners, splits, stages, most = dims
    load, relay_s, relay_r, own_s, own_r, cross_s, cross_r, back_s, back_r = sems
    experts = hidden.shape[0]
    chips = splits // 2
    me, mine = lax.axis_index("fs"), lax.axis_index("tp")
    chip, core = mine // 2, mine % 2
    pair = chip * 2 + 1 - core
    part = weights.shape[3]
    loads = []
    for q in range(stages):
        copy = pltpu.make_async_copy(
            down.at[:, :, pl.ds(q * part, part), :], weights.at[q], load.at[q]
        )
        copy.start()
        loads.append(copy)

    barrier = pltpu.get_barrier_semaphore()
    pl.semaphore_signal(barrier, device_id={"tp": pair}, device_id_type=MESH)
    for step in range(1, chips):
        other = (chip + step) % chips * 2 + core
        pl.semaphore_signal(barrier, device_id={"tp": other}, device_id_type=MESH)
    for shift in range(1, owners):
        other = (me + shift) % owners
        pl.semaphore_signal(barrier, device_id={"fs": other}, device_id_type=MESH)
    pl.semaphore_wait(barrier, chips + owners - 1)

    def block(q, column):
        total = None
        for expert in range(experts):
            term = lax.dot_general(
                hidden[expert], weights[q, expert, column], (((1,), (1,)), ((), ())),
                preferred_element_type=jnp.float32,
            )
            total = term if total is None else total + term
        return total

    def remote(source, target, send, receive, **where):
        return pltpu.make_async_remote_copy(
            src_ref=source, dst_ref=target, send_sem=send, recv_sem=receive,
            device_id=where, device_id_type=MESH,
        )

    relays, owns, crosses, backs = {}, {}, {}, {}

    def first(q):
        loads[q].wait()
        for step in range(1, chips):
            far = (chip + step) % chips * 2
            relay_out[q, step - 1] = block(q, far + 1 - core).astype(jnp.bfloat16)
            copy = remote(relay_out.at[q, step - 1], relay_in.at[q, step - 1],
                          relay_s.at[q, step - 1], relay_r.at[q, step - 1], tp=pair)
            copy.start()
            relays[q, step] = copy
        own_out[q] = block(q, pair).astype(jnp.bfloat16)
        owns[q] = remote(own_out.at[q], own_in.at[q], own_s.at[q], own_r.at[q], tp=pair)
        owns[q].start()
        for step in range(1, chips):
            far = (chip + step) % chips * 2
            relay_sum[q, step - 1] = block(q, far + core)
        for step in range(1, chips):
            far = (chip + step) % chips * 2
            relays[q, step].wait()
            both = relay_sum[q, step - 1] + relay_in[q, step - 1].astype(jnp.float32)
            cross_out[q, step - 1] = both.astype(jnp.bfloat16)
            copy = remote(cross_out.at[q, step - 1], cross_in.at[q, step - 1],
                          cross_s.at[q, step - 1], cross_r.at[q, step - 1], tp=far + core)
            copy.start()
            crosses[q, step] = copy
        own_sum[q] = block(q, mine)

    def second(q):
        owns[q].wait()
        for step in range(1, chips):
            crosses[q, step].wait()
        for shift in list(range(owners - 1, 0, -1)) + [0]:
            rows = pl.ds(shift * most, most)
            total = own_sum[q, rows] + own_in[q, rows].astype(jnp.float32)
            for step in range(1, chips):
                total += cross_in[q, step - 1, rows].astype(jnp.float32)
            total = total.astype(jnp.bfloat16)
            if shift == 0:
                back_in[q, rows] = total
                continue
            back_out[q, rows] = total
            copy = remote(back_out.at[q, rows], back_in.at[q, rows],
                          back_s.at[q, shift - 1], back_r.at[q, shift - 1],
                          fs=(me + owners - shift) % owners)
            copy.start()
            backs[q, shift] = copy

    def third(q):
        for shift in range(1, owners):
            backs[q, shift].wait()
        total = jnp.dot(pick[...], back_in[q], preferred_element_type=jnp.float32)
        out[:, pl.ds(q * part, part)] = total.astype(out.dtype)

    for turn in range(stages + 2):
        if turn < stages:
            first(turn)
        if 0 <= turn - 1 < stages:
            second(turn - 1)
        if 0 <= turn - 2 < stages:
            third(turn - 2)


def finish(hidden, down, pick, stages):
    owners, splits = lax.axis_size("fs"), lax.axis_size("tp")
    experts, slots, width = hidden.shape
    rows, features = pick.shape[0], down.shape[1] // splits
    chips, part, most = splits // 2, features // stages, slots // owners
    down = down.reshape(experts, splits, features, width)
    wide = jnp.bfloat16
    dma = pltpu.SemaphoreType.DMA
    blocks = (stages, chips - 1, slots, part)
    whole = pl.BlockSpec(memory_space=pltpu.VMEM)
    return pl.pallas_call(
        functools.partial(tail_kernel, (owners, splits, stages, most)),
        in_specs=[whole, pl.BlockSpec(memory_space=pl.ANY), whole],
        out_specs=whole,
        out_shape=jax.ShapeDtypeStruct((rows, features), wide),
        scratch_shapes=[
            pltpu.VMEM((stages, experts, splits, part, width), wide),
            pltpu.VMEM(blocks, wide),
            pltpu.VMEM(blocks, wide),
            pltpu.VMEM(blocks, jnp.float32),
            pltpu.VMEM((stages, slots, part), wide),
            pltpu.VMEM((stages, slots, part), wide),
            pltpu.VMEM((stages, slots, part), jnp.float32),
            pltpu.VMEM(blocks, wide),
            pltpu.VMEM(blocks, wide),
            pltpu.VMEM((stages, slots, part), wide),
            pltpu.VMEM((stages, slots, part), wide),
            dma((stages,)),
            dma((stages, chips - 1)),
            dma((stages, chips - 1)),
            dma((stages,)),
            dma((stages,)),
            dma((stages, chips - 1)),
            dma((stages, chips - 1)),
            dma((stages, owners - 1)),
            dma((stages, owners - 1)),
        ],
        compiler_params=pltpu.CompilerParams(
            collective_id=0, has_side_effects=True, vmem_limit_bytes=48 * 1024 * 1024
        ),
        cost_estimate=pl.CostEstimate(
            flops=2 * experts * slots * width * features * splits,
            bytes_accessed=2 * experts * features * splits * width,
            transcendentals=0,
        ),
    )(hidden, down, pick)


def chunks_of(per_owner, last):
    if per_owner % 2:
        return [(0, per_owner)]
    half = per_owner // 2
    if last and half % 2 == 0:
        return [(0, half), (half, half // 2), (half + half // 2, half // 2)]
    return [(0, half), (half, half)]


def hand_over(train, gain, chunks, number):
    owners, copies = lax.axis_size("fs"), lax.axis_size("grp")
    me, copy = lax.axis_index("fs"), lax.axis_index("grp")
    experts, rows, width = train.shape
    per_owner = experts // owners
    part = rows // copies

    def piece_for(train, shift, first, step):
        to = (me + shift) % owners
        return cast_block(train, gain, to * per_owner + first, step, copy * part, part)

    pieces = {}
    if number == 0:
        first, step = chunks[0]
        for shift in range(1, owners):
            pieces[0, shift] = piece_for(train, shift, first, step)
        early = [pieces[0, shift] for shift in range(1, owners)]
        train, early = lax.optimization_barrier((train, early))
        for shift in range(1, owners):
            pieces[0, shift] = early[shift - 1]
    serve = jnp.zeros((per_owner, owners * rows, width), jnp.bfloat16)
    own = cast_block(train, gain, me * per_owner, per_owner, 0, rows)
    serve = lax.dynamic_update_slice(serve, own, (0, me * rows, 0))
    for chunk, (first, step) in enumerate(chunks):
        late = []
        for shift in range(1, owners):
            source = (me - shift) % owners
            piece = pieces.get((chunk, shift))
            if piece is None:
                piece = piece_for(train, shift, first, step)
            piece = move(piece, "fs", shift)
            landed = [(piece, source * rows + copy * part)]
            for turn in range(1, copies):
                other = (copy - turn) % copies
                passed = move(piece, "grp", turn)
                landed.append((passed, source * rows + other * part))
            for block, row in late + landed[:1]:
                serve = lax.dynamic_update_slice(serve, block, (first, row, 0))
            late = landed[1:]
            number += 1
        for block, row in late:
            serve = lax.dynamic_update_slice(serve, block, (first, row, 0))
    return serve, number


def shards(
    tokens, route_experts, group_weight, pair_logit, norm_gain, gate_train, up_train, down_train
):
    experts, rows_here, _ = gate_train.shape
    model_width = norm_gain.shape[0]
    owners, splits = lax.axis_size("fs"), lax.axis_size("tp")
    me, my_split = lax.axis_index("fs"), lax.axis_index("tp")
    per_owner = experts // owners
    tok_rows, features = tokens.shape
    most = CAP * per_owner
    if per_owner % GROUP == 0:
        most //= 2
    most = min(most, tok_rows)
    slots = owners * most

    owner_of = (me + jnp.arange(owners, dtype=jnp.int32)) % owners
    first_gate = group_weight * jax.nn.sigmoid(pair_logit)
    second_gate = group_weight * jax.nn.sigmoid(-pair_logit)
    gates = jnp.stack([first_gate, second_gate], axis=1)
    hits = jnp.any(
        (route_experts // per_owner)[:, :, None] == owner_of[None, None, :], axis=1
    )
    counts = hits.astype(jnp.int32)
    before = jnp.cumsum(counts, axis=0) - counts
    pick = hits[:, :, None] & (
        before[:, :, None] == jnp.arange(most, dtype=jnp.int32)[None, None, :]
    )
    pick = pick.astype(jnp.bfloat16).reshape(tok_rows, slots)
    local = jnp.arange(per_owner, dtype=jnp.int32)
    named = route_experts[:, :, None, None] == (
        owner_of[:, None] * per_owner + local[None, :]
    )
    weight = jnp.sum(jnp.where(named, gates[:, :, None, None], 0.0), axis=1)
    weight = weight.reshape(tok_rows, owners * per_owner)
    high = weight.astype(jnp.bfloat16)
    low = (weight - high.astype(jnp.float32)).astype(jnp.bfloat16)
    take_rows = (((0,), (0,)), ((), ()))

    def picked(values):
        return lax.dot_general(
            pick, values, take_rows, preferred_element_type=jnp.float32
        ).astype(jnp.bfloat16)

    outgoing = picked(tokens).reshape(owners, most, features)
    levels = picked(jnp.concatenate([high, low], axis=1))
    levels = levels.reshape(owners, most, 2, owners, per_owner)
    arrived, shares = [], []
    for shift in range(owners):
        sent = outgoing[shift]
        level = levels[shift, :, :, shift].reshape(most, 2 * per_owner)
        if shift:
            level = jnp.pad(level, ((0, 0), (0, -level.shape[1] % 128)))
            sent = jnp.concatenate([sent, level], axis=1)
            sent = move(sent, "fs", shift)
            level = sent[:, features : features + 2 * per_owner]
            sent = sent[:, :features]
        arrived.append(sent)
        shares.append(level.reshape(most, 2, per_owner).astype(jnp.float32))
    arrived = jnp.concatenate(arrived, axis=0)
    shares = jnp.concatenate(shares, axis=0)
    shares = shares[:, 0] + shares[:, 1]
    section = jnp.zeros((slots, splits * features), jnp.bfloat16)
    for turn in range(splits):
        block = arrived if turn == 0 else move(arrived, "tp", turn)
        section = lax.dynamic_update_slice(
            section, block, (0, (my_split - turn) % splits * features)
        )

    gain_rows = lax.dynamic_slice_in_dim(norm_gain, me * rows_here, rows_here)
    chunks = chunks_of(per_owner, False)
    number = 0
    gate_serve, number = hand_over(gate_train, gain_rows, chunks, number)
    up_serve, number = hand_over(up_train, gain_rows, chunks, number)
    down_serve, number = hand_over(down_train, None, chunks_of(per_owner, True), number)

    squares = jnp.sum(jnp.square(section.astype(jnp.float32)), axis=1)
    row_scale = lax.rsqrt(squares / model_width + 1e-06)[:, None]
    gate_total = jnp.einsum(
        "sk,ekf->esf", section, gate_serve, preferred_element_type=jnp.float32
    )
    up_total = jnp.einsum("sk,ekf->esf", section, up_serve, preferred_element_type=jnp.float32)
    share = jnp.transpose(shares)[:, :, None]
    hidden = jax.nn.silu(row_scale * gate_total) * (row_scale * up_total) * share
    hidden = hidden.astype(jnp.bfloat16)
    stages = max(1, features // 128)
    moe_out = finish(hidden, down_serve, pick, stages)
    return (gate_serve, up_serve, down_serve, moe_out)


def solution(mesh):
    in_specs = (
        P(("grp", "fs"), "tp"),
        P(("grp", "fs"), None),
        P(("grp", "fs")),
        P(("grp", "fs")),
        P(),
        P(None, "fs", "tp"),
        P(None, "fs", "tp"),
        P(None, "fs", "tp"),
    )
    out_specs = (
        P(("grp", "fs"), None, "tp"),
        P(("grp", "fs"), None, "tp"),
        P(("grp", "fs"), None, "tp"),
        P(("grp", "fs"), "tp"),
    )

    return jax.shard_map(
        shards, mesh=mesh, in_specs=in_specs, out_specs=out_specs, check_vma=False
    )
```
